32 devices in a mesh: row: 4 (over z), col: 4 (over y, x), dp: 2 (over core).
Axes of the slice: x: 2, y: 2, z: 4, core: 2. Of those that a mesh axis runs over, the one named last changes fastest.
Arguments:
- tokens: bfloat16 [4, 16384, 1024], P('dp', ('row', 'col')), may hold values from -6 to 6
- norm_gain: float32 [1024], replicated, may hold values from 0.5 to 1.5
- in_weight: bfloat16 [1024, 512], replicated, may hold values from -0.1875 to 0.1875
- gate_weight: bfloat16 [1024, 512], replicated, may hold values from -0.1875 to 0.1875
- mix_weight: bfloat16 [512, 512], replicated, may hold values from -0.25 to 0.25
- out_weight: bfloat16 [512, 1024], replicated, may hold values from -0.25 to 0.25
Outputs:
- mixed_out: bfloat16 [4, 16384, 1024], P('dp', ('row', 'col'))
The draws below stay inside these ranges and needn't reach their ends.
All inputs are finite; a program needn't handle non-finite values.
Results may differ from the reference program's by a relative error of at most 0.007.
Values may be sent and summed in bfloat16 or wider, within the bound.
A program may use at most 128 MiB of HBM per device.

```python
import jax
import jax.numpy as jnp
from jax import lax

MODEL_WIDTH = 1024
MIX_WIDTH = 512
GROUP_WIDTH = 128
GROUPS = 4
SEQUENCES = 4
LENGTH = 16384


def block_levels(rng, extent, shards, low, largest):
    def one(position, parts):
        steps = jax.random.uniform(jax.random.fold_in(jax.random.fold_in(rng, 6), position), (parts,), jnp.float32, low / len(shards), largest / len(shards))
        return jnp.repeat(jnp.exp(steps), extent[position] // parts).reshape((-1,) + (1,) * (len(extent) - position - 1))

    level = one(*shards[0])
    for cut in shards[1:]:
        level = level * one(*cut)
    return level


def normal_values(stream_key, dims, width, bound, pieces=(), held_as=jnp.bfloat16):
    values = jax.random.normal(stream_key, dims, jnp.float32) * width
    if len(pieces) > 0:
        values = block_levels(stream_key, dims, pieces, -0.22, 0.18) * values
    return jnp.clip(values, min=-bound, max=bound).astype(held_as)


def setup_inputs(seed: int = 0) -> dict:
    splits = jax.random.split(jax.random.key(seed), 7)
    return {
        "tokens": normal_values(splits[0], (SEQUENCES, LENGTH, MODEL_WIDTH), 1.0, 6.0, ((0, 2), (1, 16))),
        "norm_gain": jnp.clip(1.0 + 0.1 * jax.random.normal(splits[1], (MODEL_WIDTH,), jnp.float32), 0.5, 1.5),
        "in_weight": normal_values(splits[2], (MODEL_WIDTH, MIX_WIDTH), MODEL_WIDTH ** -0.5, 0.1875),
        "gate_weight": normal_values(splits[3], (MODEL_WIDTH, MIX_WIDTH), MODEL_WIDTH ** -0.5, 0.1875),
        "mix_weight": normal_values(splits[4], (MIX_WIDTH, MIX_WIDTH), MIX_WIDTH ** -0.5, 0.25),
        "out_weight": normal_values(splits[5], (MIX_WIDTH, MODEL_WIDTH), MIX_WIDTH ** -0.5, 0.25),
    }


epsilon = 1e-06

def one_sequence(sequence, norm_gain, in_weight, gate_weight, mix_weight, out_weight):
    values = sequence.astype(jnp.float32)
    normed = (values * lax.rsqrt(lax.optimization_barrier(jnp.mean(values * values, axis=-1, keepdims=True)) + epsilon) * norm_gain).astype(jnp.bfloat16)
    mixed_in = jnp.dot(normed, in_weight, preferred_element_type=jnp.float32).astype(jnp.bfloat16)
    gate_values = jnp.dot(normed, gate_weight, preferred_element_type=jnp.float32).astype(jnp.bfloat16)
    grouped = mixed_in.astype(jnp.float32).reshape(LENGTH, GROUPS, GROUP_WIDTH)
    spectrum = jnp.real(jnp.fft.fft2(grouped, axes=(0, 2))) * (LENGTH * GROUP_WIDTH) ** (-0.5)
    spectrum = spectrum.reshape(LENGTH, MIX_WIDTH).astype(jnp.bfloat16)
    mixed = jnp.dot(spectrum, mix_weight, preferred_element_type=jnp.float32)
    gated_out = (mixed * jax.nn.silu(gate_values.astype(jnp.float32))).astype(jnp.bfloat16)
    return jnp.dot(gated_out, out_weight, preferred_element_type=jnp.float32).astype(jnp.bfloat16)

def reference(tokens, norm_gain, in_weight, gate_weight, mix_weight, out_weight):
    return lax.map(lambda sequence: one_sequence(sequence, norm_gain, in_weight, gate_weight, mix_weight, out_weight), tokens)
```

```python
import jax
import jax.numpy as jnp
import numpy as np
from jax import lax
from jax.sharding import PartitionSpec as P

GROUP_WIDTH = 128
LANES = 128
AXES = ("row", "col")

epsilon = 1e-06
highest = lax.Precision.HIGHEST


def angles(first_len, second_len, period):
    product = np.outer(np.arange(first_len), np.arange(second_len)) % period
    return product * (2.0 * np.pi / period)


def rms_normed(tokens, norm_gain):
    values = tokens.astype(jnp.float32)
    scaled = values * lax.rsqrt(jnp.mean(values * values, axis=-1, keepdims=True) + epsilon)
    return (scaled * norm_gain).astype(jnp.bfloat16)


def packed_in_weight(in_weight):
    model_width, mix_width = in_weight.shape
    phases = angles(GROUP_WIDTH, GROUP_WIDTH, GROUP_WIDTH)
    half = GROUP_WIDTH // 2
    table = np.where(np.arange(GROUP_WIDTH)[None, :] <= half, np.cos(phases), np.sin(phases))
    grouped = in_weight.astype(jnp.float32).reshape(model_width, -1, GROUP_WIDTH)
    packed = jnp.einsum("kgp,pq->kgq", grouped, jnp.asarray(table, jnp.float32), precision=highest)
    return packed.reshape(model_width, mix_width).astype(jnp.bfloat16)


def packed_mix_weight(mix_weight):
    half = GROUP_WIDTH // 2
    table = np.zeros((GROUP_WIDTH, GROUP_WIDTH))
    for q in range(GROUP_WIDTH):
        table[q, q] = 1.0 if q <= half else -1.0
        if q not in (0, half):
            table[q, GROUP_WIDTH - q] = 1.0
    grouped = mix_weight.reshape(-1, GROUP_WIDTH, mix_weight.shape[1])
    packed = jnp.einsum(
        "qr,grm->gqm",
        jnp.asarray(table, jnp.bfloat16),
        grouped,
        preferred_element_type=jnp.float32,
    )
    return packed.reshape(mix_weight.shape).astype(jnp.bfloat16)


def position_transform(arrived, is_sine, norm_scale):
    first_len, seq_count, share, second_len = arrived.shape
    outer = angles(first_len, first_len, first_len)
    outer_table = jnp.asarray(np.stack([np.cos(outer), -np.sin(outer)]), jnp.bfloat16)
    section = jnp.einsum("ran,nscm->rascm", outer_table, arrived, preferred_element_type=jnp.float32)
    twist = angles(first_len, second_len, first_len * second_len)
    twist_cos = jnp.asarray(np.cos(twist), jnp.float32)[:, None, None, :]
    twist_sin = jnp.asarray(np.sin(twist), jnp.float32)[:, None, None, :]
    real = section[0] * twist_cos + section[1] * twist_sin
    imag = section[1] * twist_cos - section[0] * twist_sin
    sine = is_sine[None, None, :, None]
    turned = jnp.stack([jnp.where(sine, -imag, real), jnp.where(sine, real, imag)])
    turned = turned.astype(jnp.bfloat16)
    inner = angles(second_len, second_len, second_len)
    inner_table = jnp.asarray(np.stack([np.cos(inner), np.sin(inner)]), jnp.bfloat16)
    final = jnp.einsum("rbm,rascm->bsca", inner_table, turned, preferred_element_type=jnp.float32)
    return (final * norm_scale).astype(jnp.bfloat16)


def exchange(blocks):
    return lax.all_to_all(blocks, AXES, split_axis=0, concat_axis=0, tiled=True)


def body(tokens, norm_gain, in_weight, gate_weight, mix_weight, out_weight):
    seq_count, positions, model_width = tokens.shape
    mix_width = in_weight.shape[1]
    pieces = lax.axis_size(AXES)
    length = positions * pieces
    share = mix_width // pieces
    tiles = positions // LANES
    norm_scale = (length * GROUP_WIDTH) ** (-0.5)
    normed = rms_normed(tokens, norm_gain).reshape(seq_count * positions, model_width)
    packed = lax.dot_general(
        packed_in_weight(in_weight),
        normed,
        (((0,), (1,)), ((), ())),
        preferred_element_type=jnp.float32,
    ).astype(jnp.bfloat16)
    packed = packed.reshape(pieces, share, seq_count, tiles, LANES).transpose(0, 3, 2, 1, 4)
    arrived = exchange(packed)
    gate_values = jnp.dot(normed, gate_weight, preferred_element_type=jnp.float32).astype(
        jnp.bfloat16
    )
    arrived = arrived.reshape(pieces * tiles, seq_count, share, LANES)
    column = lax.axis_index(AXES) * share + jnp.arange(share)
    is_sine = column % GROUP_WIDTH > GROUP_WIDTH // 2
    send_back = position_transform(arrived, is_sine, norm_scale)
    high_count = send_back.shape[0] // pieces
    low_count = send_back.shape[-1]
    send_back = send_back.reshape(pieces, high_count, seq_count, share, low_count)
    returned = exchange(send_back)
    mix_rows = packed_mix_weight(mix_weight).reshape(pieces, share, mix_width)
    mixed = jnp.einsum(
        "dbsca,dcm->sbam", returned, mix_rows, preferred_element_type=jnp.float32
    ).reshape(seq_count * positions, mix_width)
    gated_out = (mixed * jax.nn.silu(gate_values.astype(jnp.float32))).astype(jnp.bfloat16)
    output = jnp.dot(gated_out, out_weight, preferred_element_type=jnp.float32).astype(jnp.bfloat16)
    return output.reshape(seq_count, positions, model_width)


def solution(mesh):
    return jax.shard_map(
        body,
        mesh=mesh,
        in_specs=(P("dp", AXES, None), P(), P(), P(), P(), P()),
        out_specs=P("dp", AXES, None),
        check_vma=False,
    )
```

```python
import functools

import jax
import jax.numpy as jnp
import numpy as np
from jax import lax
from jax.experimental import pallas as pl
from jax.experimental.pallas import tpu as pltpu
from jax.sharding import PartitionSpec as P

GROUP_WIDTH = 128
LANES = 128
AXES = ("row", "col")

epsilon = 1e-06
highest = lax.Precision.HIGHEST


def angles(first_len, second_len, period):
    product = np.outer(np.arange(first_len), np.arange(second_len)) % period
    return product * (2.0 * np.pi / period)


def rms_normed(tokens, norm_gain):
    values = tokens.astype(jnp.float32)
    scaled = values * lax.rsqrt(jnp.mean(values * values, axis=-1, keepdims=True) + epsilon)
    return (scaled * norm_gain).astype(jnp.bfloat16)


def packed_in_weight(in_weight):
    model_width, mix_width = in_weight.shape
    phases = angles(GROUP_WIDTH, GROUP_WIDTH, GROUP_WIDTH)
    half = GROUP_WIDTH // 2
    table = np.where(np.arange(GROUP_WIDTH)[None, :] <= half, np.cos(phases), np.sin(phases))
    grouped = in_weight.astype(jnp.float32).reshape(model_width, -1, GROUP_WIDTH)
    packed = jnp.einsum("kgp,pq->kgq", grouped, jnp.asarray(table, jnp.float32), precision=highest)
    return packed.reshape(model_width, mix_width).astype(jnp.bfloat16)


def packed_mix_weight(mix_weight):
    half = GROUP_WIDTH // 2
    table = np.zeros((GROUP_WIDTH, GROUP_WIDTH))
    for q in range(GROUP_WIDTH):
        table[q, q] = 1.0 if q <= half else -1.0
        if q not in (0, half):
            table[q, GROUP_WIDTH - q] = 1.0
    grouped = mix_weight.reshape(-1, GROUP_WIDTH, mix_weight.shape[1])
    packed = jnp.einsum(
        "qr,grm->gqm",
        jnp.asarray(table, jnp.bfloat16),
        grouped,
        preferred_element_type=jnp.float32,
    )
    return packed.reshape(mix_weight.shape).astype(jnp.bfloat16)


def position_transform(arrived, is_sine, norm_scale):
    first_len, seq_count, share, second_len = arrived.shape
    outer = angles(first_len, first_len, first_len)
    outer_table = jnp.asarray(np.stack([np.cos(outer), -np.sin(outer)]), jnp.bfloat16)
    section = jnp.einsum("ran,nscm->rascm", outer_table, arrived, preferred_element_type=jnp.float32)
    twist = angles(first_len, second_len, first_len * second_len)
    twist_cos = jnp.asarray(np.cos(twist), jnp.float32)[:, None, None, :]
    twist_sin = jnp.asarray(np.sin(twist), jnp.float32)[:, None, None, :]
    real = section[0] * twist_cos + section[1] * twist_sin
    imag = section[1] * twist_cos - section[0] * twist_sin
    sine = is_sine[None, None, :, None]
    turned = jnp.stack([jnp.where(sine, -imag, real), jnp.where(sine, real, imag)])
    turned = turned.astype(jnp.bfloat16)
    inner = angles(second_len, second_len, second_len)
    inner_table = jnp.asarray(np.stack([np.cos(inner), np.sin(inner)]), jnp.bfloat16)
    final = jnp.einsum("rbm,rascm->bsca", inner_table, turned, preferred_element_type=jnp.float32)
    return (final * norm_scale).astype(jnp.bfloat16)


def exchange_kernel(pieces, col_count, sent_ref, out_ref, send_sems, recv_sems, own_sem):
    me = lax.axis_index("row") * col_count + lax.axis_index("col")

    def place(step):
        peer = lax.rem(me + step, pieces)
        return peer, {"row": peer // col_count, "col": peer % col_count}

    barrier = pltpu.get_barrier_semaphore()
    for step in range(1, pieces):
        pl.semaphore_signal(
            barrier, inc=1, device_id=place(step)[1], device_id_type=pl.DeviceIdType.MESH
        )
    pl.semaphore_wait(barrier, pieces - 1)
    copies = []
    for step in range(1, pieces):
        peer, where = place(step)
        copy = pltpu.make_async_remote_copy(
            src_ref=sent_ref.at[peer],
            dst_ref=out_ref.at[me],
            send_sem=send_sems.at[step],
            recv_sem=recv_sems.at[step],
            device_id=where,
            device_id_type=pl.DeviceIdType.MESH,
        )
        copy.start()
        copies.append(copy)
    own = pltpu.make_async_copy(sent_ref.at[me], out_ref.at[me], own_sem)
    own.start()
    own.wait()
    for copy in copies:
        copy.wait()


def exchange(blocks, call_id):
    pieces = blocks.shape[0]
    return pl.pallas_call(
        functools.partial(exchange_kernel, pieces, lax.axis_size("col")),
        out_shape=jax.ShapeDtypeStruct(blocks.shape, blocks.dtype),
        in_specs=[pl.BlockSpec(memory_space=pltpu.VMEM)],
        out_specs=pl.BlockSpec(memory_space=pltpu.VMEM),
        scratch_shapes=[
            pltpu.SemaphoreType.DMA((pieces,)),
            pltpu.SemaphoreType.DMA((pieces,)),
            pltpu.SemaphoreType.DMA,
        ],
        compiler_params=pltpu.CompilerParams(collective_id=call_id, has_side_effects=True),
    )(blocks)


def body(tokens, norm_gain, in_weight, gate_weight, mix_weight, out_weight):
    seq_count, positions, model_width = tokens.shape
    mix_width = in_weight.shape[1]
    pieces = lax.axis_size(AXES)
    length = positions * pieces
    share = mix_width // pieces
    tiles = positions // LANES
    norm_scale = (length * GROUP_WIDTH) ** (-0.5)
    normed = rms_normed(tokens, norm_gain).reshape(seq_count * positions, model_width)
    packed = lax.dot_general(
        packed_in_weight(in_weight),
        normed,
        (((0,), (1,)), ((), ())),
        preferred_element_type=jnp.float32,
    ).astype(jnp.bfloat16)
    packed = packed.reshape(pieces, share, seq_count, tiles, LANES).transpose(0, 3, 2, 1, 4)
    arrived = exchange(packed, 0)
    gate_values = jnp.dot(normed, gate_weight, preferred_element_type=jnp.float32).astype(
        jnp.bfloat16
    )
    arrived = arrived.reshape(pieces * tiles, seq_count, share, LANES)
    column = lax.axis_index(AXES) * share + jnp.arange(share)
    is_sine = column % GROUP_WIDTH > GROUP_WIDTH // 2
    send_back = position_transform(arrived, is_sine, norm_scale)
    high_count = send_back.shape[0] // pieces
    low_count = send_back.shape[-1]
    send_back = send_back.reshape(pieces, high_count, seq_count, share, low_count)
    returned = exchange(send_back, 1)
    mix_rows = packed_mix_weight(mix_weight).reshape(pieces, share, mix_width)
    mixed = jnp.einsum(
        "dbsca,dcm->sbam", returned, mix_rows, preferred_element_type=jnp.float32
    ).reshape(seq_count * positions, mix_width)
    gated_out = (mixed * jax.nn.silu(gate_values.astype(jnp.float32))).astype(jnp.bfloat16)
    output = jnp.dot(gated_out, out_weight, preferred_element_type=jnp.float32).astype(jnp.bfloat16)
    return output.reshape(seq_count, positions, model_width)


def solution(mesh):
    return jax.shard_map(
        body,
        mesh=mesh,
        in_specs=(P("dp", AXES, None), P(), P(), P(), P(), P()),
        out_specs=P("dp", AXES, None),
        check_vma=False,
    )
```
